32 devices in a mesh: ep: 8 (over z, y), tp: 4 (over x, core).
Axes of the slice: x: 2, y: 2, z: 4, core: 2. Of those that a mesh axis runs over, the one named last changes fastest.
Arguments:
- queries: bfloat16 [4096, 2048], P('ep', 'tp'), may hold values from -6 to 6
- forget_pre: float32 [4096, 2048], P('ep', 'tp'), may hold values from -8 to 20
- value_in: bfloat16 [4096, 2048], P('ep', 'tp'), may hold values from -6 to 6
- out_gate: bfloat16 [4096, 2048], P('ep', 'tp'), may hold values from -6 to 6
- lower_bound: float32 [2048], P('tp'), may hold values from 0.5 to 0.8
- out_gain: float32 [128], replicated, may hold values from 0.1 to 1.9
- out_weight: bfloat16 [2048, 2048], P('tp'), may hold values from -0.125 to 0.125
- moe_tokens: bfloat16 [2048, 2048], P('ep'), may hold values from -6 to 6
- moe_gain: float32 [2048], replicated, may hold values from 0.1 to 1.9
- expert_ids: int32 [2048, 4], P('ep'), may hold values from 0 to 15, all different within a row; in each aligned block of 64 rows (0 to 63, 64 to 127, ...) at most 32 rows name the same one
- route_weights: float32 [2048, 4], P('ep'), may hold values from 0.1 to 1
- w_gate: bfloat16 [16, 2048, 1024], P('ep', None, 'tp'), may hold values from -0.125 to 0.125
- w_up: bfloat16 [16, 2048, 1024], P('ep', None, 'tp'), may hold values from -0.125 to 0.125
- w_down: bfloat16 [16, 1024, 2048], P('ep', 'tp'), may hold values from -0.1875 to 0.1875
Outputs:
- mixer_out: bfloat16 [4096, 2048], P(('ep', 'tp'))
- expert_out: bfloat16 [2048, 2048], P(('ep', 'tp'))
The draws below stay inside these ranges and needn't reach their ends.
Inputs may be any that keep to these rules, and one draw needn't show every extreme that they name: `expert_ids`: each row names 4 different experts. In each aligned block of 64 rows no expert is named by more than 32 rows, and in some block some expert is named by exactly 32 rows.
All inputs are finite; a program needn't handle non-finite values.
Results may differ from the reference program's by a relative error of at most 0.01065.
Values may be sent and summed in bfloat16 or wider, within the bound.
A program may use at most 128 MiB of HBM per device.

```python
import math
import jax
import jax.numpy as jnp
import numpy as np
from jax import lax

D = 2048
HEAD_DIM = 128
BLOCK = 64
FE = 1024
EXPERTS = 16
TOPK = 4
SEQ_DEV = 512
SEQUENCE_TOTAL = 4096
MOE_ALL = 2048
QROWS = 64
CAPQ = 32
N_TP = 4


def draw_forget_pre(key, part):
    random_subkeys = jax.random.split(key, 6)
    slow_share = 0.6
    slow_mask = jax.random.uniform(random_subkeys[0], (D,)) < slow_share
    reach_factor = jax.random.uniform(random_subkeys[1], (D,), minval=0.5, maxval=2.0)
    fast_rate = 1.0 / jax.random.uniform(random_subkeys[2], (D,), minval=30.0, maxval=60.0)
    target = jnp.where(slow_mask, reach_factor / SEQUENCE_TOTAL, fast_rate)
    level_floor = jnp.log(0.35 / target)
    block_shift = jax.random.uniform(random_subkeys[3], (SEQUENCE_TOTAL // SEQ_DEV, 1), minval=-0.7, maxval=0.7)
    level_per_block = jnp.repeat(block_shift, SEQ_DEV, axis=0)
    random_noise = 0.7 * jax.random.truncated_normal(random_subkeys[4], -5.0, 5.0, (SEQUENCE_TOTAL, D))
    spike_events = jax.random.randint(random_subkeys[5], (6,), 0, SEQUENCE_TOTAL)
    position_indices = jnp.arange(SEQUENCE_TOTAL)
    spike_mask = jnp.any(position_indices[:, None] == spike_events[None, :], axis=1)
    sampled_values = jnp.where(spike_mask[:, None], -4.0 + 0.3 * random_noise, level_floor[None, :] + level_per_block + random_noise)
    return sampled_values.astype(jnp.float32)


def shard_levels(rng, extent, cuts, smallest, largest):
    def one(axis_at, parts):
        heights = jax.random.uniform(jax.random.fold_in(jax.random.fold_in(rng, 6), axis_at), (parts,), jnp.float32, smallest / len(cuts), largest / len(cuts))
        return jnp.repeat(jnp.exp(heights), extent[axis_at] // parts).reshape((-1,) + (1,) * (len(extent) - axis_at - 1))

    loudness = one(*cuts[0])
    for cut in cuts[1:]:
        loudness = loudness * one(*cut)
    return loudness


def deal_out(key, own, number, rows, count, top, bound, slope):
    ranking = jax.random.permutation(key, count)
    crowded, ordinary = shares(count, rows * top, bound, slope, True), shares(count, rows * top, bound, slope, False)
    places = jnp.arange(count)

    def named(tallies, turn):
        used = int((tallies > 0).sum())
        fixed = max(1, used // 4)
        shifted = fixed + (places - fixed + turn * (used - fixed)) % max(1, count - fixed)
        return jnp.zeros((count,), jnp.int32).at[ranking[jnp.where(places < fixed, places, shifted)]].set(jnp.asarray(tallies, jnp.int32))

    tallies = jnp.where(number % 4 == 0, named(crowded, number // 4), named(ordinary, number - number // 4 - 1))
    mixed = jax.random.permutation(jax.random.fold_in(own, 3), count)
    donor, receiver = mixed[0:count // 2 * 2:2], mixed[1:count // 2 * 2:2]
    room = jnp.minimum(tallies[donor] - 1, bound - tallies[receiver]) // 2
    room = jnp.where((donor == ranking[0]) | (receiver == ranking[0]) | (tallies[receiver] == 0), 0, jnp.maximum(room, 0))
    shifted = jax.random.randint(jax.random.fold_in(own, 4), (count // 2,), 0, 1 << 20) % (room + 1)
    tallies = tallies.at[donor].add(-shifted).at[receiver].add(shifted)
    members = jnp.searchsorted(jnp.cumsum(tallies), jnp.arange(rows * top), side="right").astype(jnp.int32)
    table = members.reshape(top, rows).T
    table = table[jax.random.permutation(jax.random.fold_in(own, 1), rows)]
    turn = jax.random.randint(jax.random.fold_in(own, 2), (rows, 1), 0, top)
    return jnp.take_along_axis(table, (jnp.arange(top)[None, :] + turn) % top, axis=1)


def shares(amount, total, reach, slope, full):
    portions = [(1 << 20) // math.isqrt(rank ** slope) + 1 for rank in range(1, amount + 1)]
    largest = reach if full else min(reach, max(-(-total // amount), total * portions[0] // sum(portions)))
    least = 1 if total - largest >= amount - 1 else 0
    counts, rest = [largest] + [least] * (amount - 1), total - largest - least * (amount - 1)
    while rest > 0:
        candidates = [i for i in range(1, amount) if counts[i] < largest] or [i for i in range(1, amount) if counts[i] < reach]
        pool, left = sum([portions[i] for i in candidates]), rest
        for i in candidates:
            more = min(reach - counts[i], max(1, left * portions[i] // pool), rest)
            counts[i] = counts[i] + more
            rest = rest - more
    return np.array(counts)


def gaussian(key, extent, spread, most, cuts=(), kind=jnp.bfloat16):
    entries = jax.random.normal(key, extent, jnp.float32) * spread
    if len(cuts) > 0:
        entries = shard_levels(key, extent, cuts, -0.22, 0.18) * entries
    return jnp.clip(entries, min=-most, max=most).astype(kind)


def setup_inputs(seed: int = 0) -> dict:
    seeds = jax.random.split(jax.random.key(seed), 15)
    queries = gaussian(seeds[0], (SEQUENCE_TOTAL, D), 1.0, 6.0, ((0, 8), (1, 4)))
    forget_pre = draw_forget_pre(jax.random.fold_in(seeds[14], 71), 0)
    value_in = gaussian(seeds[2], (SEQUENCE_TOTAL, D), 1.0, 6.0, ((0, 8), (1, 4)))
    out_gate = gaussian(seeds[3], (SEQUENCE_TOTAL, D), 1.0, 6.0, ((0, 8), (1, 4)))
    lower_bound = jnp.clip(0.5 + 0.3 * jax.random.uniform(seeds[4], (D,), jnp.float32) ** shard_levels(seeds[4], (D,), ((0, 4),), -0.2, 0.2), 0.5, 0.8)
    out_gain = jnp.clip(1.0 + 0.18 * jax.random.normal(seeds[5], (HEAD_DIM,), jnp.float32), 0.1, 1.9)
    out_weight = gaussian(seeds[6], (D, D), D ** -0.5, 0.125, ((0, 4),))
    moe_tokens = gaussian(seeds[7], (MOE_ALL, D), 1.0, 6.0, ((0, 8),))
    moe_gain = jnp.clip(1.0 + 0.18 * jax.random.normal(seeds[8], (D,), jnp.float32), 0.1, 1.9)
    expert_ids_keys = jax.random.split(jax.random.fold_in(seeds[9], 1), MOE_ALL // QROWS)
    expert_ids_turns = jax.random.permutation(jax.random.fold_in(seeds[9], 3), MOE_ALL // QROWS)
    expert_ids = jax.vmap(lambda own, number: deal_out(jax.random.fold_in(seeds[9], 2), own, number, QROWS, EXPERTS, TOPK, CAPQ, 2))(expert_ids_keys, expert_ids_turns).reshape((MOE_ALL, TOPK))
    route_weights = jnp.clip(jnp.exp(math.log(1.0) - 2.3025851 * jax.random.uniform(seeds[10], (MOE_ALL, TOPK), jnp.float32) ** shard_levels(seeds[10], (MOE_ALL, TOPK), ((0, 8),), -0.2, 0.2)), 0.1, 1.0)
    w_gate = gaussian(seeds[11], (EXPERTS, D, FE), D ** -0.5, 0.125, ((0, 8), (2, 4)))
    w_up = gaussian(seeds[12], (EXPERTS, D, FE), D ** -0.5, 0.125, ((0, 8), (2, 4)))
    w_down = gaussian(seeds[13], (EXPERTS, FE, D), FE ** -0.5, 0.1875, ((0, 8), (1, 4)))
    return dict(queries=queries, forget_pre=forget_pre, value_in=value_in, out_gate=out_gate, lower_bound=lower_bound, out_gain=out_gain, out_weight=out_weight, moe_tokens=moe_tokens, moe_gain=moe_gain, expert_ids=expert_ids, route_weights=route_weights, w_gate=w_gate, w_up=w_up, w_down=w_down)


EPS = 1e-06
HIGHEST = lax.Precision.HIGHEST

def rms_scale(values, gain):
    return values * lax.rsqrt(lax.optimization_barrier(jnp.mean(values * values, axis=-1, keepdims=True)) + EPS) * gain

def block_step(memory, inputs):
    queries_block, weight_block, values_block, forget_block = inputs
    cumulative = jnp.cumsum(forget_block, axis=1)
    length = queries_block.shape[1]
    causal = jnp.arange(length, dtype=jnp.int32)[:, None] >= jnp.arange(length, dtype=jnp.int32)[None, :]
    decayed_query = queries_block * jnp.exp(cumulative)
    decayed_key = weight_block * jnp.exp(-cumulative)
    carried_out = jnp.einsum('htd,hde->hte', decayed_query, memory, precision=HIGHEST)
    scores = jnp.einsum('htd,hsd->hts', decayed_query, decayed_key, precision=HIGHEST)
    scores = jnp.where(causal[None], scores, 0.0)
    local_out = jnp.einsum('hts,hse->hte', scores, values_block, precision=HIGHEST)
    block_total = cumulative[:, -1:, :]
    added = jnp.einsum('hsd,hse->hde', weight_block * jnp.exp(block_total - cumulative), values_block, precision=HIGHEST)
    memory = jnp.exp(block_total[:, 0, :])[:, :, None] * memory + added
    return (memory, carried_out + local_out)

def to_blocks(array, head_count):
    row_count = array.shape[0]
    return array.astype(jnp.float32).reshape(row_count // BLOCK, BLOCK, head_count, HEAD_DIM).transpose(0, 2, 1, 3)

def mixer_part(queries, forget_pre, value_in, out_gate, lower_bound, out_gain, out_weight):
    seq_rows, model_width = queries.shape
    head_count = model_width // HEAD_DIM
    weight_in = (1.0 - lower_bound) * jax.nn.sigmoid(-forget_pre)
    log_forget = jnp.log1p(-weight_in)
    start_memory = jnp.zeros((head_count, HEAD_DIM, HEAD_DIM), jnp.float32)
    final_memory, outputs = lax.scan(block_step, start_memory, (to_blocks(queries, head_count), to_blocks(weight_in, head_count), to_blocks(value_in, head_count), to_blocks(log_forget, head_count)))
    outputs = outputs.transpose(0, 2, 1, 3).reshape(seq_rows, head_count, HEAD_DIM)
    gate_act = jax.nn.silu(out_gate.astype(jnp.float32)).reshape(seq_rows, head_count, HEAD_DIM)
    gated = (rms_scale(outputs, out_gain) * gate_act).reshape(seq_rows, model_width).astype(jnp.bfloat16)
    group_width = model_width // N_TP
    summed = jnp.zeros((seq_rows, model_width), jnp.float32)
    for group_index in range(N_TP):
        low = group_index * group_width
        partial_value = jnp.dot(gated[:, low:low + group_width], out_weight[low:low + group_width], preferred_element_type=jnp.float32)
        summed = summed + lax.optimization_barrier(partial_value.astype(jnp.bfloat16)).astype(jnp.float32)
    return summed.astype(jnp.bfloat16)

def slot_ranks(ids_block, expert_count):
    onehot = (ids_block[:, :, None] == jnp.arange(expert_count, dtype=jnp.int32)[None, None, :]).astype(jnp.int32)
    return lax.optimization_barrier(jnp.sum(onehot * (jnp.cumsum(onehot, axis=1) - 1), axis=2)).astype(jnp.int32)

def experts_part(moe_tokens, moe_gain, expert_ids, route_weights, w_gate, w_up, w_down):
    token_count, model_width = moe_tokens.shape
    expert_count = w_gate.shape[0]
    hidden_units = w_gate.shape[2]
    top_count = expert_ids.shape[1]
    normed = rms_scale(moe_tokens.astype(jnp.float32), moe_gain).astype(jnp.bfloat16)
    padded = jnp.concatenate([normed, jnp.zeros((1, model_width), jnp.bfloat16)], axis=0)
    block_count = token_count // QROWS
    ids_block = expert_ids.astype(jnp.int32).reshape(block_count, QROWS * top_count)
    ranks = slot_ranks(ids_block, expert_count)
    block_base = jnp.arange(block_count, dtype=jnp.int32)[:, None] * CAPQ
    columns = (block_base + ranks).reshape(-1)
    flat_ids = ids_block.reshape(-1)
    token_index = jnp.arange(token_count * top_count, dtype=jnp.int32) // top_count
    table = jnp.full((expert_count, block_count * CAPQ), token_count, jnp.int32).at[flat_ids, columns].set(token_index)
    weight_table = jnp.zeros((expert_count, block_count * CAPQ), jnp.float32).at[flat_ids, columns].set(route_weights.reshape(-1))
    group_units = hidden_units // N_TP

    def one_expert(summed, inputs):
        rows_index, weights_now, gate_matrix, up_matrix, down_matrix = inputs
        rows_now = padded[rows_index]
        gate_pre = jnp.dot(rows_now, gate_matrix, preferred_element_type=jnp.float32)
        up_pre = jnp.dot(rows_now, up_matrix, preferred_element_type=jnp.float32)
        hidden = (jax.nn.silu(gate_pre) * up_pre).astype(jnp.bfloat16)
        total_rows = jnp.zeros((rows_now.shape[0], model_width), jnp.float32)
        for group_index in range(N_TP):
            low = group_index * group_units
            partial_value = jnp.dot(hidden[:, low:low + group_units], down_matrix[low:low + group_units], preferred_element_type=jnp.float32)
            total_rows = total_rows + lax.optimization_barrier(partial_value.astype(jnp.bfloat16)).astype(jnp.float32)
        expert_rows = lax.optimization_barrier(total_rows.astype(jnp.bfloat16)).astype(jnp.float32)
        return (summed.at[rows_index].add(expert_rows * weights_now[:, None]), None)
    start_sum = jnp.zeros((token_count + 1, model_width), jnp.float32)
    summed, unused = lax.scan(one_expert, start_sum, (table, weight_table, w_gate, w_up, w_down))
    return summed[:token_count].astype(jnp.bfloat16)

def reference(queries, forget_pre, value_in, out_gate, lower_bound, out_gain, out_weight, moe_tokens, moe_gain, expert_ids, route_weights, w_gate, w_up, w_down):
    mixer_out = mixer_part(queries, forget_pre, value_in, out_gate, lower_bound, out_gain, out_weight)
    expert_out = experts_part(moe_tokens, moe_gain, expert_ids, route_weights, w_gate, w_up, w_down)
    return (mixer_out, expert_out)
```

```python
import jax
import jax.numpy as jnp
from jax import lax
from jax.experimental import pallas as pl
from jax.experimental.pallas import tpu as pltpu
from jax.sharding import PartitionSpec as P

HEAD_DIM = 128
BLOCK = 64


EPS = 1e-06
HIGHEST = lax.Precision.HIGHEST


def rms_scale(values, gain):
    return values * lax.rsqrt(jnp.mean(values * values, axis=-1, keepdims=True) + EPS) * gain


def slot_ranks(ids_block, expert_count):
    onehot = (
        ids_block[:, :, None] == jnp.arange(expert_count, dtype=jnp.int32)[None, None, :]
    ).astype(jnp.int32)
    return jnp.sum(onehot * (jnp.cumsum(onehot, axis=1) - 1), axis=2)


MESH = pl.DeviceIdType.MESH
VMEM = pl.BlockSpec(memory_space=pltpu.VMEM)


def remote(source, target, send, receive, device):
    return pltpu.make_async_remote_copy(
        src_ref=source,
        dst_ref=target,
        send_sem=send,
        recv_sem=receive,
        device_id=device,
        device_id_type=MESH,
    )


def flip(value):
    return value + 1 - 2 * (value % 2)


def fused_kernel(
    tok_hbm,
    gain_ref,
    ids_ref,
    route_ref,
    wg_hbm,
    wu_hbm,
    wd_hbm,
    query_hbm,
    forget_hbm,
    value_hbm,
    gate_hbm,
    bound_ref,
    ogain_ref,
    ow_hbm,
    mix_out,
    moe_out,
    wg,
    wu,
    wd,
    query,
    forget,
    value,
    ogate,
    ow,
    held,
    part,
    other,
    sums,
    bx,
    by,
    cx,
    cy,
    zr,
    wbuf,
    cum,
    near,
    qdec,
    gated,
    mpart,
    mother,
    msum,
    mx,
    st,
    sz,
    tables,
    columns,
    send,
    recv,
    lsem,
):
    f32, bf16 = jnp.float32, jnp.bfloat16
    ep = lax.axis_index("ep")
    tp = lax.axis_index("tp")
    z, y = ep // 2, ep % 2
    x, c = tp // 2, tp % 2
    planes, _, quarters, piece, width = held.shape
    seq, chans = forget.shape
    heads = chans // HEAD_DIM
    top = ids_ref.shape[0]
    local_experts, _, hidden_units = wg.shape
    xfirst = bx.shape[2]
    xrows, yrows = pl.ds(0, xfirst), pl.ds(xfirst, piece - xfirst)
    fold = piece // 2
    low_half, high_half = pl.ds(0, fold), pl.ds(fold, piece - fold)
    partner = (ep, flip(tp))
    xn = (ep, (tp + 2) % 4)
    yn = (flip(ep), tp)
    others = (z, flip(z), (z + 2) % 4, 3 - z)
    zn = [(others[k] * 2 + y, tp) for k in range(planes)]

    def spot(dx, dc):
        return pl.ds(pl.multiple_of((((x + dx) % 2) * 2 + (c + dc) % 2) * piece, piece), piece)

    own_loads = []
    for dc in range(2):
        for dx in range(2):
            own_loads.append(
                pltpu.make_async_copy(
                    tok_hbm.at[spot(dx, dc)], held.at[0, dc, dx], lsem.at[8 + len(own_loads)]
                )
            )
            own_loads[-1].start()
    loads = {}
    for at, (name, source, target) in enumerate(
        (
            ("forget", forget_hbm, forget),
            ("value", value_hbm, value),
            ("query", query_hbm, query),
            ("wg", wg_hbm, wg),
            ("wu", wu_hbm, wu),
            ("wd", wd_hbm, wd),
            ("gate", gate_hbm, ogate),
            ("ow", ow_hbm, ow),
        )
    ):
        loads[name] = pltpu.make_async_copy(source, target, lsem.at[at])
        loads[name].start()

    peers = [partner, xn, yn] + zn[1:]
    barrier = pltpu.get_barrier_semaphore()
    for device in peers:
        pl.semaphore_signal(barrier, inc=1, device_id=device, device_id_type=MESH)

    copies = {}

    def put(name, source, target, device):
        at = len(copies)
        copies[name] = remote(source, target, send.at[at], recv.at[at], device)
        copies[name].start()

    def got(*names):
        for name in names:
            copies[name].wait_recv()

    def ready(*names):
        for name in names:
            if name in loads:
                loads.pop(name).wait()

    def run_experts(block, table, store):
        ready("wg", "wu", "wd")
        tokens = rms_scale(block.astype(f32), gain_ref[...]).astype(bf16)
        hidden = []
        for expert in range(local_experts):
            chosen = table[:, :top] == (ep * local_experts + expert).astype(f32)
            weight = jnp.sum(
                jnp.where(chosen, table[:, top : 2 * top], 0.0), axis=1, keepdims=True
            )
            gate = jnp.dot(tokens, wg[expert], preferred_element_type=f32)
            up = jnp.dot(tokens, wu[expert], preferred_element_type=f32)
            hidden.append((jax.nn.silu(gate) * up * weight).astype(bf16))
        hidden = jnp.concatenate(hidden, axis=1)
        down = wd[...].reshape(local_experts * hidden_units, width)
        step = min(width, 512)
        for low in range(0, width, step):
            total = jnp.dot(hidden, down[:, low : low + step], preferred_element_type=f32)
            store(low, step, total.astype(bf16))

    def experts_own(dy):
        if dy == 1:
            got("down0", "down1", "ty0")
        else:
            for load in own_loads:
                load.wait()
        columns[0, dy] = jnp.transpose(tables[0, dy])
        table = jnp.concatenate(
            [columns[0, dy, spot(dx, dc)] for dc in range(2) for dx in range(2)], axis=0
        )

        def store(low, step, total):
            part[0, :, 2 * dy : 2 * dy + 2, :, low : low + step] = total.reshape(2, 2, piece, step)

        block = held[0, :, 2 * dy : 2 * dy + 2].reshape(4 * piece, width)
        run_experts(block, table, store)
        if dy == 1:
            put("r10", part.at[0, 1], other.at[0], partner)

    shown = []

    def experts_plane(k, side):
        if side == 1:
            got(*[f"d{q}{k}" for q in range(quarters)])
        if k not in shown:
            shown.append(k)
            got(f"ty{k}")
            for dy in range(2):
                columns[k, dy] = jnp.transpose(tables[k, dy])
        table = jnp.concatenate(
            [columns[k, dy, spot(dx, side)] for dy in range(2) for dx in range(2)], axis=0
        )

        def store(low, step, total):
            part[k, side, :, :, low : low + step] = total.reshape(quarters, piece, step)

        run_experts(held[k, side].reshape(quarters * piece, width), table, store)
        if side == 1:
            put(f"r1{k}", part.at[k, 1], other.at[k], partner)

    def start():
        tables[0, 0, :top] = ids_ref[...].astype(f32)
        tables[0, 0, top : 2 * top] = route_ref[...]
        pl.semaphore_wait(barrier, len(peers))
        for load in own_loads[:2]:
            load.wait()
        del own_loads[:2]
        put("z1", held.at[0, 0, 0], held.at[1, 0, 0], zn[1])
        put("own0", held.at[0, 0, 0], held.at[0, 0, 2], yn)
        put("own1", held.at[0, 0, 1], held.at[0, 0, 3], yn)
        for k in range(1, planes):
            put(f"tz{k}", tables.at[0, 0], tables.at[k, 0], zn[k])
        put("ty0", tables.at[0, 0], tables.at[0, 1], yn)

    def far(k):
        put(f"z{k}", held.at[0, 0, 0], held.at[k, 0, 0], zn[k])

    def own():
        for dx in range(2):
            got(f"own{dx}")
            put(f"down{dx}", held.at[0, 0, 2 + dx], held.at[0, 1, 2 + dx], partner)

    def plane(k):
        got(f"z{k}")
        mine = held.at[k, 0, 0]
        put(f"x{k}", mine, held.at[k, 0, 1], xn)
        put(f"y{k}", mine, held.at[k, 0, 2], yn)
        put(f"d0{k}", mine, held.at[k, 1, 0], partner)
        got(f"tz{k}")
        put(f"ty{k}", tables.at[k, 0], tables.at[k, 1], yn)

    def from_x(k):
        got(f"x{k}")
        put(f"fy{k}", held.at[k, 0, 1, low_half], held.at[k, 0, 3, low_half], yn)
        put(f"d1{k}", held.at[k, 0, 1], held.at[k, 1, 1], partner)

    def from_y(k):
        got(f"y{k}")
        put(f"fx{k}", held.at[k, 0, 2, high_half], held.at[k, 0, 3, high_half], xn)
        put(f"d2{k}", held.at[k, 0, 2], held.at[k, 1, 2], partner)

    def corner(k):
        got(f"fy{k}", f"fx{k}")
        put(f"d3{k}", held.at[k, 0, 3], held.at[k, 1, 3], partner)

    def add(*terms):
        total = terms[0].astype(f32)
        for term in terms[1:]:
            total = total + term.astype(f32)
        return total.astype(bf16)

    def rs_first(k):
        got(f"r1{k}")

        def body(q, carry):
            sums[k, q % 2, q // 2] = add(part[k, 0, q], other[k, q])
            return carry

        lax.fori_loop(0, quarters, body, 0)
        put(f"r2x{k}", sums.at[k, 1, :, xrows], bx.at[k], xn)
        put(f"r2y{k}", sums.at[k, :, 1, yrows], by.at[k], yn)

    def rs_x(k):
        got(f"r2x{k}")
        for dy in (1, 0):
            sums[k, 0, dy, :xfirst] = add(sums[k, 0, dy, :xfirst], bx[k, dy])
            if dy == 1:
                put(f"r3y{k}", sums.at[k, 0, 1, xrows], cy.at[k], yn)

    def rs_y(k):
        got(f"r2y{k}")
        for dx in (1, 0):
            sums[k, dx, 0, xfirst:] = add(sums[k, dx, 0, xfirst:], by[k, dx])
            if dx == 1:
                put(f"r3x{k}", sums.at[k, 1, 0, yrows], cx.at[k], xn)

    def rs_third(k):
        got(f"r3y{k}", f"r3x{k}")
        sums[k, 0, 0, :xfirst] = add(sums[k, 0, 0, :xfirst], cy[k])
        sums[k, 0, 0, xfirst:] = add(sums[k, 0, 0, xfirst:], cx[k])
        if k > 0:
            put(f"r4{k}", sums.at[k, 0, 0], zr.at[k - 1], zn[k])

    def rs_end():
        got(*[f"r4{k}" for k in range(1, planes)])
        moe_out[...] = add(sums[0, 0, 0], *[zr[k] for k in range(planes - 1)])

    def mix_decay():
        ready("forget")
        tile = min(seq, 256)
        row = lax.broadcasted_iota(jnp.int32, (tile, tile), 0)
        col = lax.broadcasted_iota(jnp.int32, (tile, tile), 1)
        ones = jnp.where((row >= col) & (row // BLOCK == col // BLOCK), 1.0, 0.0).astype(bf16)
        for low in range(0, seq, tile):
            weight = (1.0 - bound_ref[...]) * jax.nn.sigmoid(-forget[low : low + tile])
            logs = jnp.log1p(-weight)
            high = logs.astype(bf16)
            rest = (logs - high.astype(f32)).astype(bf16)
            wbuf[low : low + tile] = weight
            cum[low : low + tile] = jnp.dot(ones, high, preferred_element_type=f32) + jnp.dot(
                ones, rest, preferred_element_type=f32
            )

    def dot_of(left, right, left_dim, right_dim):
        return lax.dot_general(
            left, right, (((left_dim,), (right_dim,)), ((), ())), preferred_element_type=f32
        )

    def mix_local(first, last):
        ready("value", "query")
        lower = lax.broadcasted_iota(jnp.int32, (BLOCK, BLOCK), 0) >= lax.broadcasted_iota(
            jnp.int32, (BLOCK, BLOCK), 1
        )

        def body(head, carry):
            lanes = pl.ds(pl.multiple_of(head * HEAD_DIM, HEAD_DIM), HEAD_DIM)
            memory, before = None, None
            for low in range(0, seq, BLOCK):
                rows = pl.ds(low, BLOCK)
                cumulative = cum[rows, lanes]
                total = jnp.exp(cumulative[BLOCK - 1 :])
                values = value[rows, lanes]
                raised = wbuf[rows, lanes] * jnp.exp(-cumulative)
                decayed = query[rows, lanes].astype(f32) * jnp.exp(cumulative)
                decayed_low = decayed.astype(bf16)
                scores = dot_of(decayed_low, raised.astype(bf16), 1, 1)
                scores = jnp.where(lower, scores, 0.0).astype(bf16)
                result = dot_of(scores, values, 1, 0)
                added = dot_of(values, (raised * total).astype(bf16), 0, 0)
                if memory is None:
                    qdec[rows, lanes] = decayed_low
                    memory, before = added, total
                else:
                    result += dot_of(decayed_low, memory.astype(bf16), 1, 1)
                    qdec[rows, lanes] = (decayed * before).astype(bf16)
                    memory, before = memory * total + added, before * total
                near[rows, lanes] = result
            store_state(st.at[0, head], memory, before)
            return carry

        lax.fori_loop(first, last, body, 0)

    def store_state(target, memory, decay):
        decay = jnp.broadcast_to(decay, (16, HEAD_DIM))
        high = decay.astype(bf16).astype(f32)
        top = lax.broadcasted_iota(jnp.int32, decay.shape, 0) < 8
        target[:HEAD_DIM] = memory.astype(bf16)
        target[HEAD_DIM:] = jnp.where(top, high, decay - high).astype(bf16)

    def load_state(source):
        tail = source[HEAD_DIM:].astype(f32)
        return source[:HEAD_DIM].astype(f32), tail[0:1] + tail[8:9]

    upper = y.astype(f32)

    def state_plane():
        put("sy", st.at[0], st.at[1], yn)

    def state_combine():
        got("sy")

        def body(head, carry):
            mine, mine_decay = load_state(st.at[0, head])
            theirs, theirs_decay = load_state(st.at[1, head])
            early = mine + upper * (theirs - mine)
            late = theirs + upper * (mine - theirs)
            late_decay = theirs_decay + upper * (mine_decay - theirs_decay)
            store_state(sz.at[0, head], early * late_decay + late, mine_decay * theirs_decay)
            return carry

        lax.fori_loop(0, heads, body, 0)
        for k in range(1, planes):
            put(f"sz{k}", sz.at[0], sz.at[k], zn[k])

    def mix_finish():
        got(*[f"sz{k}" for k in range(1, planes)])
        ready("gate")

        def body(head, carry):
            lanes = pl.ds(pl.multiple_of(head * HEAD_DIM, HEAD_DIM), HEAD_DIM)
            memory = jnp.zeros((HEAD_DIM, HEAD_DIM), f32)
            for place in range(planes - 1):
                keep = jnp.where(z > place, 1.0, 0.0)
                state, decay = load_state(sz.at[others[place], head])
                memory = memory * (decay * keep + (1.0 - keep)) + state * keep
            state, decay = load_state(st.at[1, head])
            memory = memory * (decay * upper + (1.0 - upper)) + state * upper
            result = near[:, lanes] + dot_of(qdec[:, lanes], memory.astype(bf16), 1, 1)
            gate = jax.nn.silu(ogate[:, lanes].astype(f32))
            gated[:, lanes] = (rms_scale(result, ogain_ref[...]) * gate).astype(bf16)
            return carry

        lax.fori_loop(0, heads, body, 0)

    def mix_project():
        ready("ow")
        lanes, rows = mpart.shape[:2]
        step = min(width, 512)
        for low in range(0, width, step):
            total = jnp.dot(gated[...], ow[:, low : low + step], preferred_element_type=f32)
            mpart[:, :, low : low + step] = total.astype(bf16).reshape(lanes, rows, step)
        for dx in (1, 0):
            there = (x + dx) % 2
            put(f"m1{dx}", mpart.at[2 * there + 1 - c], mother.at[dx], partner)

    def mix_cross():
        got("m11")
        msum[...] = add(mpart[2 * (1 - x) + c], mother[1])
        put("m2", msum, mx, xn)

    def mix_end():
        got("m10", "m2")
        mix_out[...] = add(mpart[2 * x + c], mother[0], mx[...])

    start()
    far(3)
    plane(1)
    mix_decay()
    plane(3)
    experts_own(0)
    far(2)
    mix_local(0, heads // 2)
    from_y(1)
    from_x(3)
    from_y(3)
    plane(2)
    from_x(1)
    mix_local(heads // 2, heads)
    corner(3)
    own()
    state_plane()
    experts_plane(3, 0)
    experts_plane(3, 1)
    from_y(2)
    corner(1)
    from_x(2)
    rs_first(3)
    experts_plane(1, 1)
    state_combine()
    experts_plane(1, 0)
    rs_first(1)
    corner(2)
    experts_plane(2, 0)
    experts_plane(2, 1)
    rs_y(3)
    rs_x(3)
    experts_own(1)
    rs_x(1)
    rs_first(2)
    rs_third(3)
    rs_y(1)
    rs_x(2)
    rs_first(0)
    rs_third(1)
    mix_finish()
    mix_project()
    rs_y(2)
    rs_x(0)
    mix_cross()
    rs_third(2)
    rs_y(0)
    mix_end()
    rs_third(0)
    rs_end()
    for copy in copies.values():
        copy.wait_send()


def hand_over(mixed, routed, mix_out, moe_out):
    mix_out[...] = mixed[...]
    moe_out[...] = routed[...]


def fused(
    queries,
    forget_pre,
    value_in,
    out_gate,
    lower_bound,
    out_gain,
    out_weight,
    moe_tokens,
    moe_gain,
    expert_ids,
    route_weights,
    w_gate,
    w_up,
    w_down,
    planes,
    lanes,
):
    bf16, f32 = jnp.bfloat16, jnp.float32
    seq, chans = queries.shape
    heads = chans // HEAD_DIM
    rows, width = moe_tokens.shape
    piece = rows // lanes
    top = expert_ids.shape[1]
    xfirst = piece // 2
    slot = (piece, width)
    vmem, dma = pltpu.VMEM, pltpu.SemaphoreType.DMA
    count = 80
    flops = 2 * rows * planes * 2 * w_gate.size * 3
    anywhere = pl.BlockSpec(memory_space=pl.ANY)
    mixed, routed = pl.pallas_call(
        fused_kernel,
        out_shape=(
            jax.ShapeDtypeStruct((seq // lanes, width), bf16),
            jax.ShapeDtypeStruct(slot, bf16),
        ),
        in_specs=[
            anywhere, VMEM, VMEM, VMEM, anywhere, anywhere, anywhere,
            anywhere, anywhere, anywhere, anywhere, VMEM, VMEM, anywhere,
        ],
        out_specs=(VMEM, VMEM),
        scratch_shapes=[
            vmem(w_gate.shape, bf16),
            vmem(w_up.shape, bf16),
            vmem(w_down.shape, bf16),
            vmem((seq, chans), bf16),
            vmem((seq, chans), f32),
            vmem((seq, chans), bf16),
            vmem((seq, chans), bf16),
            vmem((chans, width), bf16),
            vmem((planes, 2, 4, piece, width), bf16),
            vmem((planes, 2, 4, piece, width), bf16),
            vmem((planes, 4, piece, width), bf16),
            vmem((planes, 2, 2, piece, width), bf16),
            vmem((planes, 2, xfirst, width), bf16),
            vmem((planes, 2, piece - xfirst, width), bf16),
            vmem((planes, piece - xfirst, width), bf16),
            vmem((planes, xfirst, width), bf16),
            vmem((planes - 1, piece, width), bf16),
            vmem((seq, chans), f32),
            vmem((seq, chans), f32),
            vmem((seq, chans), f32),
            vmem((seq, chans), bf16),
            vmem((seq, chans), bf16),
            vmem((lanes, seq // lanes, width), bf16),
            vmem((2, seq // lanes, width), bf16),
            vmem((seq // lanes, width), bf16),
            vmem((seq // lanes, width), bf16),
            vmem((2, heads, HEAD_DIM + 16, HEAD_DIM), bf16),
            vmem((planes, heads, HEAD_DIM + 16, HEAD_DIM), bf16),
            vmem((planes, 2, 2 * top, rows), f32),
            vmem((planes, 2, rows, 2 * top), f32),
            dma((count,)),
            dma((count,)),
            dma((12,)),
        ],
        compiler_params=pltpu.CompilerParams(
            collective_id=0, has_side_effects=True, vmem_limit_bytes=63 * 2**20
        ),
        cost_estimate=pl.CostEstimate(
            flops=flops, bytes_accessed=100 * 2**20, transcendentals=0
        ),
        name="fused",
    )(
        moe_tokens,
        moe_gain[None],
        expert_ids.T,
        route_weights.T,
        w_gate,
        w_up,
        w_down,
        queries,
        forget_pre,
        value_in,
        out_gate,
        lower_bound[None],
        out_gain[None],
        out_weight,
    )
    return pl.pallas_call(
        hand_over,
        out_shape=tuple(jax.ShapeDtypeStruct(a.shape, a.dtype) for a in (mixed, routed)),
        in_specs=[VMEM, VMEM],
        out_specs=(VMEM, VMEM),
        name="hand_over",
    )(mixed, routed)


def contract(left, right, left_dim, right_dim):
    return lax.dot_general(
        left,
        right,
        (((left_dim,), (right_dim,)), ((), ())),
        precision=HIGHEST,
        preferred_element_type=jnp.float32,
    )


def decay_blocks(forget, bound):
    weight = (1.0 - bound) * jax.nn.sigmoid(-forget)
    logs = jnp.log1p(-weight)
    lower = (
        lax.broadcasted_iota(jnp.int32, (BLOCK, BLOCK), 0)
        >= lax.broadcasted_iota(jnp.int32, (BLOCK, BLOCK), 1)
    )
    ones = jnp.where(lower, 1.0, 0.0)
    blocks = []
    for low in range(0, forget.shape[0], BLOCK):
        cumulative = contract(ones, logs[low : low + BLOCK], 1, 0)
        total = cumulative[BLOCK - 1 :]
        blocks.append((weight[low : low + BLOCK], cumulative, total))
    return lower, blocks


def state_kernel(forget_ref, value_ref, bound_ref, out_ref):
    _, blocks = decay_blocks(forget_ref[...], bound_ref[...])
    memory, span = None, None
    for at, (weight, cumulative, total) in enumerate(blocks):
        values = value_ref[at * BLOCK : (at + 1) * BLOCK].astype(jnp.float32)
        added = contract(values, weight * jnp.exp(total - cumulative), 0, 0)
        memory = added if memory is None else memory * jnp.exp(total) + added
        span = total if span is None else span + total
    decay = jnp.broadcast_to(jnp.exp(span), (16, HEAD_DIM))
    high = decay.astype(jnp.bfloat16).astype(jnp.float32)
    first = lax.broadcasted_iota(jnp.int32, decay.shape, 0) < 8
    out_ref[0, :HEAD_DIM] = memory.astype(jnp.bfloat16)
    out_ref[0, HEAD_DIM:] = jnp.where(first, high, decay - high).astype(jnp.bfloat16)


def mixer_kernel(
    states_ref, query_ref, forget_ref, value_ref, gate_ref, bound_ref, gain_ref, out_ref
):
    def one(hop, memory):
        tail = states_ref[hop, 0, HEAD_DIM:].astype(jnp.float32)
        return memory * (tail[0:1] + tail[8:9]) + states_ref[hop, 0, :HEAD_DIM].astype(jnp.float32)

    memory = lax.fori_loop(
        0, lax.axis_index("ep"), one, jnp.zeros((HEAD_DIM, HEAD_DIM), jnp.float32)
    )
    lower, blocks = decay_blocks(forget_ref[...], bound_ref[...])
    for at, (weight, cumulative, total) in enumerate(blocks):
        rows = slice(at * BLOCK, (at + 1) * BLOCK)
        values = value_ref[rows].astype(jnp.float32)
        decayed_query = query_ref[rows].astype(jnp.float32) * jnp.exp(cumulative)
        scores = contract(decayed_query, weight * jnp.exp(-cumulative), 1, 1)
        result = contract(jnp.where(lower, scores, 0.0), values, 1, 0)
        result += contract(decayed_query, memory, 1, 1)
        added = contract(values, weight * jnp.exp(total - cumulative), 0, 0)
        memory = memory * jnp.exp(total) + added
        gate = jax.nn.silu(gate_ref[rows].astype(jnp.float32))
        out_ref[rows] = (rms_scale(result, gain_ref[...]) * gate).astype(jnp.bfloat16)


def head_block(rows):
    return pl.BlockSpec((rows, HEAD_DIM), lambda head: (0, head))


def head_states(forget_pre, value_in, lower_bound):
    rows, width = forget_pre.shape
    heads = width // HEAD_DIM
    return pl.pallas_call(
        state_kernel,
        grid=(heads,),
        out_shape=jax.ShapeDtypeStruct((heads, HEAD_DIM + 16, HEAD_DIM), jnp.bfloat16),
        in_specs=[head_block(rows), head_block(rows), head_block(1)],
        out_specs=pl.BlockSpec((1, HEAD_DIM + 16, HEAD_DIM), lambda head: (head, 0, 0)),
        cost_estimate=pl.CostEstimate(
            flops=10**9, bytes_accessed=8 * forget_pre.size, transcendentals=0
        ),
        name="head_states",
    )(forget_pre, value_in, lower_bound[None])


def mix_heads(states, queries, forget_pre, value_in, out_gate, lower_bound, out_gain):
    rows, width = forget_pre.shape
    heads = width // HEAD_DIM
    count = states.shape[0]
    return pl.pallas_call(
        mixer_kernel,
        grid=(heads,),
        out_shape=jax.ShapeDtypeStruct((rows, width), jnp.bfloat16),
        in_specs=[
            pl.BlockSpec((count, 1, HEAD_DIM + 16, HEAD_DIM), lambda head: (0, head, 0, 0)),
            head_block(rows),
            head_block(rows),
            head_block(rows),
            head_block(rows),
            head_block(1),
            pl.BlockSpec((1, HEAD_DIM), lambda head: (0, 0)),
        ],
        out_specs=head_block(rows),
        cost_estimate=pl.CostEstimate(
            flops=4 * 10**9, bytes_accessed=16 * forget_pre.size, transcendentals=0
        ),
        name="mix_heads",
    )(states, queries, forget_pre, value_in, out_gate, lower_bound[None], out_gain[None])


def sparse_experts(
    moe_tokens, moe_gain, expert_ids, route_weights, w_gate, w_up, w_down, model_width
):
    lanes = lax.axis_size("tp")
    lane_index = lax.axis_index("tp")
    ep_count = lax.axis_size("ep")
    qrows = moe_tokens.shape[0] // lanes
    top_count = expert_ids.shape[1]
    local_experts = w_gate.shape[0]
    expert_count = local_experts * ep_count
    capacity = max(2, 2 * qrows * top_count // expert_count)
    send_tokens = lax.dynamic_slice_in_dim(moe_tokens, lane_index * qrows, qrows, 0)
    send_ids = lax.dynamic_slice_in_dim(expert_ids, lane_index * qrows, qrows, 0)
    quarters = send_tokens.shape[0] // qrows
    normed = rms_scale(send_tokens.astype(jnp.float32), moe_gain).astype(jnp.bfloat16)
    ids_block = send_ids.reshape(quarters, qrows * top_count)
    ranks = slot_ranks(ids_block, expert_count)
    quarter_base = jnp.arange(quarters, dtype=jnp.int32)[:, None] * (expert_count * capacity)
    slot_index = (quarter_base + ids_block * capacity + ranks).reshape(-1)
    source_row = jnp.arange(quarters * qrows * top_count, dtype=jnp.int32) // top_count
    sources = (
        jnp.full((quarters * expert_count * capacity,), quarters * qrows, jnp.int32)
        .at[slot_index]
        .set(source_row)
    )
    padded = jnp.concatenate([normed, jnp.zeros((1, model_width), jnp.bfloat16)], axis=0)
    outgoing = padded[sources].reshape(quarters, ep_count, local_experts * capacity, model_width)
    arrived = lax.all_to_all(outgoing, "ep", split_axis=1, concat_axis=1, tiled=True)
    piece = lax.all_gather(arrived, "tp", axis=0, tiled=True)
    shaped = piece.reshape(piece.shape[0], ep_count, local_experts, capacity, model_width)
    gate_pre = jnp.einsum("qsecd,edf->qsecf", shaped, w_gate, preferred_element_type=jnp.float32)
    up_pre = jnp.einsum("qsecd,edf->qsecf", shaped, w_up, preferred_element_type=jnp.float32)
    hidden = (jax.nn.silu(gate_pre) * up_pre).astype(jnp.bfloat16)
    lane_rows = ep_count * local_experts * capacity
    projected = jnp.einsum("qsecf,efd->qsecd", hidden, w_down, preferred_element_type=jnp.float32)
    expert_sum = lax.psum_scatter(
        projected.reshape(lax.axis_size("tp") * lane_rows, model_width).astype(jnp.bfloat16),
        "tp",
        scatter_dimension=0,
        tiled=True,
    )
    leaving = expert_sum.reshape(ep_count, local_experts * capacity, model_width)
    returned = lax.all_to_all(leaving, "ep", split_axis=0, concat_axis=0, tiled=True)
    returned = returned.reshape(expert_count * capacity, model_width)
    own_quarter = lane_index * (quarters // lanes)
    own_ids = lax.dynamic_index_in_dim(ids_block, own_quarter, 0, keepdims=False)
    own_ranks = lax.dynamic_index_in_dim(ranks, own_quarter, 0, keepdims=False)
    picked = (
        returned[own_ids * capacity + own_ranks]
        .astype(jnp.float32)
        .reshape(qrows, top_count, model_width)
    )
    own_weights = lax.dynamic_slice_in_dim(route_weights, lane_index * qrows, qrows, 0)
    expert_out = jnp.sum(picked * own_weights[:, :, None], axis=1).astype(jnp.bfloat16)
    return expert_out


def local(
    queries,
    forget_pre,
    value_in,
    out_gate,
    lower_bound,
    out_gain,
    out_weight,
    moe_tokens,
    moe_gain,
    expert_ids,
    route_weights,
    w_gate,
    w_up,
    w_down,
):
    lanes = lax.axis_size("tp")
    ep_count = lax.axis_size("ep")
    model_width = out_weight.shape[1]
    tokens, top_count = expert_ids.shape
    dense_slots = 2 * (tokens // lanes) * top_count * lanes
    if lanes == 4 and ep_count == 8 and tokens * ep_count <= dense_slots:
        return fused(
            queries,
            forget_pre,
            value_in,
            out_gate,
            lower_bound,
            out_gain,
            out_weight,
            moe_tokens,
            moe_gain,
            expert_ids,
            route_weights,
            w_gate,
            w_up,
            w_down,
            ep_count // 2,
            lanes,
        )
    packed = head_states(forget_pre, value_in, lower_bound)
    gathered = lax.all_gather(packed, "ep")
    gated = mix_heads(
        gathered, queries, forget_pre, value_in, out_gate, lower_bound, out_gain
    )
    mixer_part = jnp.dot(gated, out_weight, preferred_element_type=jnp.float32).astype(
        jnp.bfloat16
    )
    mixer_sum = lax.psum_scatter(mixer_part, "tp", scatter_dimension=0, tiled=True)
    expert_out = sparse_experts(
        moe_tokens, moe_gain, expert_ids, route_weights, w_gate, w_up, w_down, model_width
    )
    return (mixer_sum, expert_out)


def solution(mesh):
    in_specs = (
        P("ep", "tp"),
        P("ep", "tp"),
        P("ep", "tp"),
        P("ep", "tp"),
        P("tp"),
        P(),
        P("tp", None),
        P("ep", None),
        P(),
        P("ep", None),
        P("ep", None),
        P("ep", None, "tp"),
        P("ep", None, "tp"),
        P("ep", "tp", None),
    )
    out_specs = (P(("ep", "tp"), None), P(("ep", "tp"), None))
    return jax.shard_map(local, mesh=mesh, in_specs=in_specs, out_specs=out_specs, check_vma=False)
```

```python
import jax
import jax.numpy as jnp
from jax import lax
from jax.experimental import pallas as pl
from jax.experimental.pallas import tpu as pltpu
from jax.sharding import PartitionSpec as P

HEAD_DIM = 128
BLOCK = 64


EPS = 1e-06
X_SHARE = (2, 4, 4, 4)
HIGHEST = lax.Precision.HIGHEST


def rms_scale(values, gain):
    return values * lax.rsqrt(jnp.mean(values * values, axis=-1, keepdims=True) + EPS) * gain


def slot_ranks(ids_block, expert_count):
    onehot = (
        ids_block[:, :, None] == jnp.arange(expert_count, dtype=jnp.int32)[None, None, :]
    ).astype(jnp.int32)
    return jnp.sum(onehot * (jnp.cumsum(onehot, axis=1) - 1), axis=2)


MESH = pl.DeviceIdType.MESH
VMEM = pl.BlockSpec(memory_space=pltpu.VMEM)


def remote(source, target, send, receive, device):
    return pltpu.make_async_remote_copy(
        src_ref=source,
        dst_ref=target,
        send_sem=send,
        recv_sem=receive,
        device_id=device,
        device_id_type=MESH,
    )


def flip(value):
    return value + 1 - 2 * (value % 2)


def fused_kernel(
    tok_hbm,
    gain_hbm,
    ids_hbm,
    route_hbm,
    wg_hbm,
    wu_hbm,
    wd_hbm,
    query_hbm,
    forget_hbm,
    value_hbm,
    gate_hbm,
    bound_hbm,
    ogain_hbm,
    ow_hbm,
    mix_out,
    moe_out,
    gain_ref,
    ids_ref,
    route_ref,
    bound_ref,
    ogain_ref,
    wg,
    wu,
    wd,
    query,
    forget,
    value,
    ogate,
    ow,
    held,
    part,
    other,
    sums,
    bx,
    by,
    cx,
    cy,
    zr,
    wbuf,
    cum,
    near,
    qdec,
    gated,
    mpart,
    mother,
    msum,
    mx,
    st,
    sz,
    tables,
    columns,
    send,
    recv,
    lsem,
):
    f32, bf16 = jnp.float32, jnp.bfloat16
    ep = lax.axis_index("ep")
    tp = lax.axis_index("tp")
    z, y = ep // 2, ep % 2
    x, c = tp // 2, tp % 2
    planes, _, quarters, piece, width = held.shape
    seq, chans = forget.shape
    heads = chans // HEAD_DIM
    top = ids_hbm.shape[0]
    local_experts, _, hidden_units = wg.shape
    xfirst = [piece * share // 8 for share in X_SHARE]
    ysize = [piece - rows for rows in xfirst]
    fold = piece // 2
    low_half, high_half = pl.ds(0, fold), pl.ds(fold, piece - fold)
    partner = (ep, flip(tp))
    xn = (ep, (tp + 2) % 4)
    yn = (flip(ep), tp)
    others = (z, flip(z), (z + 2) % 4, 3 - z)
    zn = [(others[k] * 2 + y, tp) for k in range(planes)]

    peers = [partner, xn, yn] + zn[1:]
    barrier = pltpu.get_barrier_semaphore()
    for device in peers:
        pl.semaphore_signal(barrier, inc=1, device_id=device, device_id_type=MESH)

    def spot(dx, dc):
        return pl.ds(pl.multiple_of((((x + dx) % 2) * 2 + (c + dc) % 2) * piece, piece), piece)

    own_loads = []
    for dc in range(2):
        for dx in range(2):
            own_loads.append(
                pltpu.make_async_copy(
                    tok_hbm.at[spot(dx, dc)], held.at[0, dc, dx], lsem.at[13 + len(own_loads)]
                )
            )
            own_loads[-1].start()
    loads = {}
    for at, (name, source, target) in enumerate(
        (
            ("ids", ids_hbm, ids_ref),
            ("route", route_hbm, route_ref),
            ("bound", bound_hbm, bound_ref),
            ("forget", forget_hbm, forget),
            ("value", value_hbm, value),
            ("query", query_hbm, query),
            ("gain", gain_hbm, gain_ref),
            ("wg", wg_hbm, wg),
            ("wu", wu_hbm, wu),
            ("wd", wd_hbm, wd),
            ("gate", gate_hbm, ogate),
            ("ogain", ogain_hbm, ogain_ref),
            ("ow", ow_hbm, ow),
        )
    ):
        loads[name] = pltpu.make_async_copy(source, target, lsem.at[at])
        loads[name].start()

    copies = {}

    def put(name, source, target, device):
        at = len(copies)
        copies[name] = remote(source, target, send.at[at], recv.at[at], device)
        copies[name].start()

    def got(*names):
        for name in names:
            copies[name].wait_recv()

    def ready(*names):
        for name in names:
            if name in loads:
                loads.pop(name).wait()

    def run_experts(block, table, store):
        ready("gain", "wg", "wu", "wd")
        tokens = rms_scale(block.astype(f32), gain_ref[...]).astype(bf16)
        hidden = []
        for expert in range(local_experts):
            chosen = table[:, :top] == (ep * local_experts + expert).astype(f32)
            weight = jnp.sum(
                jnp.where(chosen, table[:, top : 2 * top], 0.0), axis=1, keepdims=True
            )
            gate = jnp.dot(tokens, wg[expert], preferred_element_type=f32)
            up = jnp.dot(tokens, wu[expert], preferred_element_type=f32)
            hidden.append((jax.nn.silu(gate) * up * weight).astype(bf16))
        hidden = jnp.concatenate(hidden, axis=1)
        down = wd[...].reshape(local_experts * hidden_units, width)
        step = min(width, 512)
        for low in range(0, width, step):
            total = jnp.dot(hidden, down[:, low : low + step], preferred_element_type=f32)
            store(low, step, total.astype(bf16))

    def experts_own(dy):
        if dy == 1:
            got("down0", "down1", "ty0")
        else:
            for load in own_loads:
                load.wait()
        columns[0, dy] = jnp.transpose(tables[0, dy])
        table = jnp.concatenate(
            [columns[0, dy, spot(dx, dc)] for dc in range(2) for dx in range(2)], axis=0
        )

        def store(low, step, total):
            part[0, :, 2 * dy : 2 * dy + 2, :, low : low + step] = total.reshape(2, 2, piece, step)

        block = held[0, :, 2 * dy : 2 * dy + 2].reshape(4 * piece, width)
        run_experts(block, table, store)
        if dy == 1:
            put("r10", part.at[0, 1], other.at[0], partner)

    shown = []

    def experts_plane(k, side):
        if side == 1:
            got(*[f"d{q}{k}" for q in range(quarters)])
        if k not in shown:
            shown.append(k)
            got(f"ty{k}")
            for dy in range(2):
                columns[k, dy] = jnp.transpose(tables[k, dy])
        table = jnp.concatenate(
            [columns[k, dy, spot(dx, side)] for dy in range(2) for dx in range(2)], axis=0
        )

        def store(low, step, total):
            part[k, side, :, :, low : low + step] = total.reshape(quarters, piece, step)

        run_experts(held[k, side].reshape(quarters * piece, width), table, store)
        if side == 1:
            put(f"r1{k}", part.at[k, 1], other.at[k], partner)

    def start():
        pl.semaphore_wait(barrier, len(peers))
        for load in own_loads[:2]:
            load.wait()
        del own_loads[:2]
        put("z1", held.at[0, 0, 0], held.at[1, 0, 0], zn[1])
        put("own0", held.at[0, 0, 0], held.at[0, 0, 2], yn)
        put("own1", held.at[0, 0, 1, low_half], held.at[0, 0, 3, low_half], yn)
        ready("ids", "route")
        tables[0, 0, :top] = ids_ref[...].astype(f32)
        tables[0, 0, top : 2 * top] = route_ref[...]
        for k in range(1, planes):
            put(f"tz{k}", tables.at[0, 0], tables.at[k, 0], zn[k])
        put("ty0", tables.at[0, 0], tables.at[0, 1], yn)

    def far(k):
        put(f"z{k}", held.at[0, 0, 0], held.at[k, 0, 0], zn[k])

    def own(dx):
        got(f"own{dx}")
        if dx == 0:
            put("ownx", held.at[0, 0, 2, high_half], held.at[0, 0, 3, high_half], xn)
        else:
            got("ownx")
        put(f"down{dx}", held.at[0, 0, 2 + dx], held.at[0, 1, 2 + dx], partner)

    def plane(k):
        got(f"z{k}")
        mine = held.at[k, 0, 0]
        put(f"x{k}", mine, held.at[k, 0, 1], xn)
        put(f"y{k}", mine, held.at[k, 0, 2], yn)
        put(f"d0{k}", mine, held.at[k, 1, 0], partner)
        got(f"tz{k}")
        put(f"ty{k}", tables.at[k, 0], tables.at[k, 1], yn)

    def from_x(k):
        got(f"x{k}")
        put(f"fy{k}", held.at[k, 0, 1, low_half], held.at[k, 0, 3, low_half], yn)
        put(f"d1{k}", held.at[k, 0, 1], held.at[k, 1, 1], partner)

    def from_y(k):
        got(f"y{k}")
        put(f"fx{k}", held.at[k, 0, 2, high_half], held.at[k, 0, 3, high_half], xn)
        put(f"d2{k}", held.at[k, 0, 2], held.at[k, 1, 2], partner)

    def corner(k):
        got(f"fy{k}", f"fx{k}")
        put(f"d3{k}", held.at[k, 0, 3], held.at[k, 1, 3], partner)

    def add(*terms):
        total = terms[0].astype(f32)
        for term in terms[1:]:
            total = total + term.astype(f32)
        return total.astype(bf16)

    def rs_first(k):
        got(f"r1{k}")
        xf, ys = xfirst[k], ysize[k]

        def body(q, carry):
            sums[k, q % 2, q // 2] = add(part[k, 0, q], other[k, q])
            return carry

        lax.fori_loop(0, quarters, body, 0)
        put(f"r2x{k}", sums.at[k, 1, :, pl.ds(0, xf)], bx.at[k, :, pl.ds(0, xf)], xn)
        put(f"r2y{k}", sums.at[k, :, 1, pl.ds(xf, ys)], by.at[k, :, pl.ds(0, ys)], yn)

    def rs_x(k):
        got(f"r2x{k}")
        xf = xfirst[k]
        for dy in (1, 0):
            sums[k, 0, dy, :xf] = add(sums[k, 0, dy, :xf], bx[k, dy, :xf])
            if dy == 1:
                put(f"r3y{k}", sums.at[k, 0, 1, pl.ds(0, xf)], cy.at[k, pl.ds(0, xf)], yn)

    def rs_y(k):
        got(f"r2y{k}")
        xf, ys = xfirst[k], ysize[k]
        for dx in (1, 0):
            sums[k, dx, 0, xf:] = add(sums[k, dx, 0, xf:], by[k, dx, :ys])
            if dx == 1:
                put(f"r3x{k}", sums.at[k, 1, 0, pl.ds(xf, ys)], cx.at[k, pl.ds(0, ys)], xn)

    def rs_third(k):
        got(f"r3y{k}", f"r3x{k}")
        xf, ys = xfirst[k], ysize[k]
        sums[k, 0, 0, :xf] = add(sums[k, 0, 0, :xf], cy[k, :xf])
        sums[k, 0, 0, xf:] = add(sums[k, 0, 0, xf:], cx[k, :ys])
        if k > 0:
            put(f"r4{k}", sums.at[k, 0, 0], zr.at[k - 1], zn[k])

    def rs_end():
        got(*[f"r4{k}" for k in range(1, planes)])
        moe_out[...] = add(sums[0, 0, 0], *[zr[k] for k in range(planes - 1)])

    def mix_decay():
        ready("forget", "bound")
        tile = min(seq, 256)
        row = lax.broadcasted_iota(jnp.int32, (tile, tile), 0)
        col = lax.broadcasted_iota(jnp.int32, (tile, tile), 1)
        ones = jnp.where((row >= col) & (row // BLOCK == col // BLOCK), 1.0, 0.0).astype(bf16)
        for low in range(0, seq, tile):
            weight = (1.0 - bound_ref[...]) * jax.nn.sigmoid(-forget[low : low + tile])
            logs = jnp.log1p(-weight)
            high = logs.astype(bf16)
            rest = (logs - high.astype(f32)).astype(bf16)
            wbuf[low : low + tile] = weight
            cum[low : low + tile] = jnp.dot(ones, high, preferred_element_type=f32) + jnp.dot(
                ones, rest, preferred_element_type=f32
            )

    def dot_of(left, right, left_dim, right_dim):
        return lax.dot_general(
            left, right, (((left_dim,), (right_dim,)), ((), ())), preferred_element_type=f32
        )

    def mix_local(first, last):
        ready("value", "query")
        lower = lax.broadcasted_iota(jnp.int32, (BLOCK, BLOCK), 0) >= lax.broadcasted_iota(
            jnp.int32, (BLOCK, BLOCK), 1
        )

        def body(head, carry):
            lanes = pl.ds(pl.multiple_of(head * HEAD_DIM, HEAD_DIM), HEAD_DIM)
            memory, before = None, None
            for low in range(0, seq, BLOCK):
                rows = pl.ds(low, BLOCK)
                cumulative = cum[rows, lanes]
                total = jnp.exp(cumulative[BLOCK - 1 :])
                values = value[rows, lanes]
                raised = wbuf[rows, lanes] * jnp.exp(-cumulative)
                decayed = query[rows, lanes].astype(f32) * jnp.exp(cumulative)
                decayed_low = decayed.astype(bf16)
                scores = dot_of(decayed_low, raised.astype(bf16), 1, 1)
                scores = jnp.where(lower, scores, 0.0).astype(bf16)
                result = dot_of(scores, values, 1, 0)
                added = dot_of(values, (raised * total).astype(bf16), 0, 0)
                if memory is None:
                    qdec[rows, lanes] = decayed_low
                    memory, before = added, total
                else:
                    result += dot_of(decayed_low, memory.astype(bf16), 1, 1)
                    qdec[rows, lanes] = (decayed * before).astype(bf16)
                    memory, before = memory * total + added, before * total
                near[rows, lanes] = result
            store_state(st.at[0, head], memory, before)
            return carry

        lax.fori_loop(first, last, body, 0)

    def store_state(target, memory, decay):
        decay = jnp.broadcast_to(decay, (16, HEAD_DIM))
        high = decay.astype(bf16).astype(f32)
        top = lax.broadcasted_iota(jnp.int32, decay.shape, 0) < 8
        target[:HEAD_DIM] = memory.astype(bf16)
        target[HEAD_DIM:] = jnp.where(top, high, decay - high).astype(bf16)

    def load_state(source):
        tail = source[HEAD_DIM:].astype(f32)
        return source[:HEAD_DIM].astype(f32), tail[0:1] + tail[8:9]

    upper = y.astype(f32)

    def state_plane():
        put("sy", st.at[0], st.at[1], yn)

    def state_combine():
        got("sy")

        def body(head, carry):
            mine, mine_decay = load_state(st.at[0, head])
            theirs, theirs_decay = load_state(st.at[1, head])
            early = mine + upper * (theirs - mine)
            late = theirs + upper * (mine - theirs)
            late_decay = theirs_decay + upper * (mine_decay - theirs_decay)
            store_state(sz.at[0, head], early * late_decay + late, mine_decay * theirs_decay)
            return carry

        lax.fori_loop(0, heads, body, 0)
        for k in range(1, planes):
            put(f"sz{k}", sz.at[0], sz.at[k], zn[k])

    def mix_finish():
        got(*[f"sz{k}" for k in range(1, planes)])
        ready("gate", "ogain")

        def body(head, carry):
            lanes = pl.ds(pl.multiple_of(head * HEAD_DIM, HEAD_DIM), HEAD_DIM)
            memory = jnp.zeros((HEAD_DIM, HEAD_DIM), f32)
            for place in range(planes - 1):
                keep = jnp.where(z > place, 1.0, 0.0)
                state, decay = load_state(sz.at[others[place], head])
                memory = memory * (decay * keep + (1.0 - keep)) + state * keep
            state, decay = load_state(st.at[1, head])
            memory = memory * (decay * upper + (1.0 - upper)) + state * upper
            result = near[:, lanes] + dot_of(qdec[:, lanes], memory.astype(bf16), 1, 1)
            gate = jax.nn.silu(ogate[:, lanes].astype(f32))
            gated[:, lanes] = (rms_scale(result, ogain_ref[...]) * gate).astype(bf16)
            return carry

        lax.fori_loop(0, heads, body, 0)

    def mix_project():
        ready("ow")
        lanes, rows = mpart.shape[:2]
        step = min(width, 512)
        for low in range(0, width, step):
            total = jnp.dot(gated[...], ow[:, low : low + step], preferred_element_type=f32)
            mpart[:, :, low : low + step] = total.astype(bf16).reshape(lanes, rows, step)
        for dx in (1, 0):
            there = (x + dx) % 2
            put(f"m1{dx}", mpart.at[2 * there + 1 - c], mother.at[dx], partner)

    def mix_cross():
        got("m11")
        msum[...] = add(mpart[2 * (1 - x) + c], mother[1])
        put("m2", msum, mx, xn)

    def mix_end():
        got("m10", "m2")
        mix_out[...] = add(mpart[2 * x + c], mother[0], mx[...])

    start()
    far(3)
    mix_decay()
    own(0)
    mix_local(0, heads // 2)
    plane(1)
    plane(3)
    experts_own(0)
    far(2)
    from_x(1)
    from_y(3)
    from_x(3)
    from_y(1)
    plane(2)
    mix_local(heads // 2, heads)
    corner(3)
    state_plane()
    experts_plane(3, 0)
    experts_plane(3, 1)
    corner(1)
    from_y(2)
    from_x(2)
    rs_first(3)
    experts_plane(1, 1)
    own(1)
    state_combine()
    experts_plane(1, 0)
    rs_first(1)
    corner(2)
    experts_plane(2, 1)
    rs_y(3)
    rs_x(3)
    experts_plane(2, 0)
    rs_first(2)
    rs_y(1)
    rs_x(1)
    experts_own(1)
    mix_finish()
    rs_third(3)
    rs_x(2)
    rs_first(0)
    rs_y(2)
    mix_project()
    rs_third(1)
    mix_cross()
    rs_third(2)
    rs_y(0)
    mix_end()
    rs_x(0)
    rs_third(0)
    rs_end()
    for copy in copies.values():
        copy.wait_send()


def hand_over(mixed, routed, mix_out, moe_out):
    mix_out[...] = mixed[...]
    moe_out[...] = routed[...]


def fused(
    queries,
    forget_pre,
    value_in,
    out_gate,
    lower_bound,
    out_gain,
    out_weight,
    moe_tokens,
    moe_gain,
    expert_ids,
    route_weights,
    w_gate,
    w_up,
    w_down,
    planes,
    lanes,
):
    bf16, f32 = jnp.bfloat16, jnp.float32
    seq, chans = queries.shape
    heads = chans // HEAD_DIM
    rows, width = moe_tokens.shape
    piece = rows // lanes
    top = expert_ids.shape[1]
    xmost = max(X_SHARE) * piece // 8
    ymost = piece - min(X_SHARE) * piece // 8
    slot = (piece, width)
    vmem, dma = pltpu.VMEM, pltpu.SemaphoreType.DMA
    count = 80
    flops = 2 * rows * planes * 2 * w_gate.size * 3
    anywhere = pl.BlockSpec(memory_space=pltpu.HBM)
    mixed, routed = pl.pallas_call(
        fused_kernel,
        out_shape=(
            jax.ShapeDtypeStruct((seq // lanes, width), bf16),
            jax.ShapeDtypeStruct(slot, bf16),
        ),
        in_specs=[
            anywhere, anywhere, anywhere, anywhere, anywhere, anywhere, anywhere,
            anywhere, anywhere, anywhere, anywhere, anywhere, anywhere, anywhere,
        ],
        out_specs=(VMEM, VMEM),
        scratch_shapes=[
            vmem((1, width), f32),
            vmem((top, rows), jnp.int32),
            vmem((top, rows), f32),
            vmem((1, chans), f32),
            vmem((1, HEAD_DIM), f32),
            vmem(w_gate.shape, bf16),
            vmem(w_up.shape, bf16),
            vmem(w_down.shape, bf16),
            vmem((seq, chans), bf16),
            vmem((seq, chans), f32),
            vmem((seq, chans), bf16),
            vmem((seq, chans), bf16),
            vmem((chans, width), bf16),
            vmem((planes, 2, 4, piece, width), bf16),
            vmem((planes, 2, 4, piece, width), bf16),
            vmem((planes, 4, piece, width), bf16),
            vmem((planes, 2, 2, piece, width), bf16),
            vmem((planes, 2, xmost, width), bf16),
            vmem((planes, 2, ymost, width), bf16),
            vmem((planes, ymost, width), bf16),
            vmem((planes, xmost, width), bf16),
            vmem((planes - 1, piece, width), bf16),
            vmem((seq, chans), f32),
            vmem((seq, chans), f32),
            vmem((seq, chans), f32),
            vmem((seq, chans), bf16),
            vmem((seq, chans), bf16),
            vmem((lanes, seq // lanes, width), bf16),
            vmem((2, seq // lanes, width), bf16),
            vmem((seq // lanes, width), bf16),
            vmem((seq // lanes, width), bf16),
            vmem((2, heads, HEAD_DIM + 16, HEAD_DIM), bf16),
            vmem((planes, heads, HEAD_DIM + 16, HEAD_DIM), bf16),
            vmem((planes, 2, 2 * top, rows), f32),
            vmem((planes, 2, rows, 2 * top), f32),
            dma((count,)),
            dma((count,)),
            dma((17,)),
        ],
        compiler_params=pltpu.CompilerParams(
            collective_id=0, has_side_effects=True, vmem_limit_bytes=63 * 2**20
        ),
        cost_estimate=pl.CostEstimate(
            flops=flops, bytes_accessed=100 * 2**20, transcendentals=0
        ),
        name="fused",
    )(
        moe_tokens,
        moe_gain[None],
        expert_ids.T,
        route_weights.T,
        w_gate,
        w_up,
        w_down,
        queries,
        forget_pre,
        value_in,
        out_gate,
        lower_bound[None],
        out_gain[None],
        out_weight,
    )
    return pl.pallas_call(
        hand_over,
        out_shape=tuple(jax.ShapeDtypeStruct(a.shape, a.dtype) for a in (mixed, routed)),
        in_specs=[VMEM, VMEM],
        out_specs=(VMEM, VMEM),
        name="hand_over",
    )(mixed, routed)


def contract(left, right, left_dim, right_dim):
    return lax.dot_general(
        left,
        right,
        (((left_dim,), (right_dim,)), ((), ())),
        precision=HIGHEST,
        preferred_element_type=jnp.float32,
    )


def decay_blocks(forget, bound):
    weight = (1.0 - bound) * jax.nn.sigmoid(-forget)
    logs = jnp.log1p(-weight)
    lower = (
        lax.broadcasted_iota(jnp.int32, (BLOCK, BLOCK), 0)
        >= lax.broadcasted_iota(jnp.int32, (BLOCK, BLOCK), 1)
    )
    ones = jnp.where(lower, 1.0, 0.0)
    blocks = []
    for low in range(0, forget.shape[0], BLOCK):
        cumulative = contract(ones, logs[low : low + BLOCK], 1, 0)
        total = cumulative[BLOCK - 1 :]
        blocks.append((weight[low : low + BLOCK], cumulative, total))
    return lower, blocks


def state_kernel(forget_ref, value_ref, bound_ref, out_ref):
    _, blocks = decay_blocks(forget_ref[...], bound_ref[...])
    memory, span = None, None
    for at, (weight, cumulative, total) in enumerate(blocks):
        values = value_ref[at * BLOCK : (at + 1) * BLOCK].astype(jnp.float32)
        added = contract(values, weight * jnp.exp(total - cumulative), 0, 0)
        memory = added if memory is None else memory * jnp.exp(total) + added
        span = total if span is None else span + total
    decay = jnp.broadcast_to(jnp.exp(span), (16, HEAD_DIM))
    high = decay.astype(jnp.bfloat16).astype(jnp.float32)
    first = lax.broadcasted_iota(jnp.int32, decay.shape, 0) < 8
    out_ref[0, :HEAD_DIM] = memory.astype(jnp.bfloat16)
    out_ref[0, HEAD_DIM:] = jnp.where(first, high, decay - high).astype(jnp.bfloat16)


def mixer_kernel(
    states_ref, query_ref, forget_ref, value_ref, gate_ref, bound_ref, gain_ref, out_ref
):
    def one(hop, memory):
        tail = states_ref[hop, 0, HEAD_DIM:].astype(jnp.float32)
        return memory * (tail[0:1] + tail[8:9]) + states_ref[hop, 0, :HEAD_DIM].astype(jnp.float32)

    memory = lax.fori_loop(
        0, lax.axis_index("ep"), one, jnp.zeros((HEAD_DIM, HEAD_DIM), jnp.float32)
    )
    lower, blocks = decay_blocks(forget_ref[...], bound_ref[...])
    for at, (weight, cumulative, total) in enumerate(blocks):
        rows = slice(at * BLOCK, (at + 1) * BLOCK)
        values = value_ref[rows].astype(jnp.float32)
        decayed_query = query_ref[rows].astype(jnp.float32) * jnp.exp(cumulative)
        scores = contract(decayed_query, weight * jnp.exp(-cumulative), 1, 1)
        result = contract(jnp.where(lower, scores, 0.0), values, 1, 0)
        result += contract(decayed_query, memory, 1, 1)
        added = contract(values, weight * jnp.exp(total - cumulative), 0, 0)
        memory = memory * jnp.exp(total) + added
        gate = jax.nn.silu(gate_ref[rows].astype(jnp.float32))
        out_ref[rows] = (rms_scale(result, gain_ref[...]) * gate).astype(jnp.bfloat16)


def head_block(rows):
    return pl.BlockSpec((rows, HEAD_DIM), lambda head: (0, head))


def head_states(forget_pre, value_in, lower_bound):
    rows, width = forget_pre.shape
    heads = width // HEAD_DIM
    return pl.pallas_call(
        state_kernel,
        grid=(heads,),
        out_shape=jax.ShapeDtypeStruct((heads, HEAD_DIM + 16, HEAD_DIM), jnp.bfloat16),
        in_specs=[head_block(rows), head_block(rows), head_block(1)],
        out_specs=pl.BlockSpec((1, HEAD_DIM + 16, HEAD_DIM), lambda head: (head, 0, 0)),
        cost_estimate=pl.CostEstimate(
            flops=10**9, bytes_accessed=8 * forget_pre.size, transcendentals=0
        ),
        name="head_states",
    )(forget_pre, value_in, lower_bound[None])


def mix_heads(states, queries, forget_pre, value_in, out_gate, lower_bound, out_gain):
    rows, width = forget_pre.shape
    heads = width // HEAD_DIM
    count = states.shape[0]
    return pl.pallas_call(
        mixer_kernel,
        grid=(heads,),
        out_shape=jax.ShapeDtypeStruct((rows, width), jnp.bfloat16),
        in_specs=[
            pl.BlockSpec((count, 1, HEAD_DIM + 16, HEAD_DIM), lambda head: (0, head, 0, 0)),
            head_block(rows),
            head_block(rows),
            head_block(rows),
            head_block(rows),
            head_block(1),
            pl.BlockSpec((1, HEAD_DIM), lambda head: (0, 0)),
        ],
        out_specs=head_block(rows),
        cost_estimate=pl.CostEstimate(
            flops=4 * 10**9, bytes_accessed=16 * forget_pre.size, transcendentals=0
        ),
        name="mix_heads",
    )(states, queries, forget_pre, value_in, out_gate, lower_bound[None], out_gain[None])


def sparse_experts(
    moe_tokens, moe_gain, expert_ids, route_weights, w_gate, w_up, w_down, model_width
):
    lanes = lax.axis_size("tp")
    lane_index = lax.axis_index("tp")
    ep_count = lax.axis_size("ep")
    qrows = moe_tokens.shape[0] // lanes
    top_count = expert_ids.shape[1]
    local_experts = w_gate.shape[0]
    expert_count = local_experts * ep_count
    capacity = max(2, 2 * qrows * top_count // expert_count)
    send_tokens = lax.dynamic_slice_in_dim(moe_tokens, lane_index * qrows, qrows, 0)
    send_ids = lax.dynamic_slice_in_dim(expert_ids, lane_index * qrows, qrows, 0)
    quarters = send_tokens.shape[0] // qrows
    normed = rms_scale(send_tokens.astype(jnp.float32), moe_gain).astype(jnp.bfloat16)
    ids_block = send_ids.reshape(quarters, qrows * top_count)
    ranks = slot_ranks(ids_block, expert_count)
    quarter_base = jnp.arange(quarters, dtype=jnp.int32)[:, None] * (expert_count * capacity)
    slot_index = (quarter_base + ids_block * capacity + ranks).reshape(-1)
    source_row = jnp.arange(quarters * qrows * top_count, dtype=jnp.int32) // top_count
    sources = (
        jnp.full((quarters * expert_count * capacity,), quarters * qrows, jnp.int32)
        .at[slot_index]
        .set(source_row)
    )
    padded = jnp.concatenate([normed, jnp.zeros((1, model_width), jnp.bfloat16)], axis=0)
    outgoing = padded[sources].reshape(quarters, ep_count, local_experts * capacity, model_width)
    arrived = lax.all_to_all(outgoing, "ep", split_axis=1, concat_axis=1, tiled=True)
    piece = lax.all_gather(arrived, "tp", axis=0, tiled=True)
    shaped = piece.reshape(piece.shape[0], ep_count, local_experts, capacity, model_width)
    gate_pre = jnp.einsum("qsecd,edf->qsecf", shaped, w_gate, preferred_element_type=jnp.float32)
    up_pre = jnp.einsum("qsecd,edf->qsecf", shaped, w_up, preferred_element_type=jnp.float32)
    hidden = (jax.nn.silu(gate_pre) * up_pre).astype(jnp.bfloat16)
    lane_rows = ep_count * local_experts * capacity
    projected = jnp.einsum("qsecf,efd->qsecd", hidden, w_down, preferred_element_type=jnp.float32)
    expert_sum = lax.psum_scatter(
        projected.reshape(lax.axis_size("tp") * lane_rows, model_width).astype(jnp.bfloat16),
        "tp",
        scatter_dimension=0,
        tiled=True,
    )
    leaving = expert_sum.reshape(ep_count, local_experts * capacity, model_width)
    returned = lax.all_to_all(leaving, "ep", split_axis=0, concat_axis=0, tiled=True)
    returned = returned.reshape(expert_count * capacity, model_width)
    own_quarter = lane_index * (quarters // lanes)
    own_ids = lax.dynamic_index_in_dim(ids_block, own_quarter, 0, keepdims=False)
    own_ranks = lax.dynamic_index_in_dim(ranks, own_quarter, 0, keepdims=False)
    picked = (
        returned[own_ids * capacity + own_ranks]
        .astype(jnp.float32)
        .reshape(qrows, top_count, model_width)
    )
    own_weights = lax.dynamic_slice_in_dim(route_weights, lane_index * qrows, qrows, 0)
    expert_out = jnp.sum(picked * own_weights[:, :, None], axis=1).astype(jnp.bfloat16)
    return expert_out


def local(
    queries,
    forget_pre,
    value_in,
    out_gate,
    lower_bound,
    out_gain,
    out_weight,
    moe_tokens,
    moe_gain,
    expert_ids,
    route_weights,
    w_gate,
    w_up,
    w_down,
):
    lanes = lax.axis_size("tp")
    ep_count = lax.axis_size("ep")
    model_width = out_weight.shape[1]
    tokens, top_count = expert_ids.shape
    dense_slots = 2 * (tokens // lanes) * top_count * lanes
    if lanes == 4 and ep_count == 8 and tokens * ep_count <= dense_slots:
        return fused(
            queries,
            forget_pre,
            value_in,
            out_gate,
            lower_bound,
            out_gain,
            out_weight,
            moe_tokens,
            moe_gain,
            expert_ids,
            route_weights,
            w_gate,
            w_up,
            w_down,
            ep_count // 2,
            lanes,
        )
    packed = head_states(forget_pre, value_in, lower_bound)
    gathered = lax.all_gather(packed, "ep")
    gated = mix_heads(
        gathered, queries, forget_pre, value_in, out_gate, lower_bound, out_gain
    )
    mixer_part = jnp.dot(gated, out_weight, preferred_element_type=jnp.float32).astype(
        jnp.bfloat16
    )
    mixer_sum = lax.psum_scatter(mixer_part, "tp", scatter_dimension=0, tiled=True)
    expert_out = sparse_experts(
        moe_tokens, moe_gain, expert_ids, route_weights, w_gate, w_up, w_down, model_width
    )
    return (mixer_sum, expert_out)


def solution(mesh):
    in_specs = (
        P("ep", "tp"),
        P("ep", "tp"),
        P("ep", "tp"),
        P("ep", "tp"),
        P("tp"),
        P(),
        P("tp", None),
        P("ep", None),
        P(),
        P("ep", None),
        P("ep", None),
        P("ep", None, "tp"),
        P("ep", None, "tp"),
        P("ep", "tp", None),
    )
    out_specs = (P(("ep", "tp"), None), P(("ep", "tp"), None))
    return jax.shard_map(local, mesh=mesh, in_specs=in_specs, out_specs=out_specs, check_vma=False)
```
